32 devices in a mesh: grp: 2 (over y), sp: 4 (over z), fs: 2 (over x), tp: 2 (over core).
Axes of the slice: x: 2, y: 2, z: 4, core: 2. Of those that a mesh axis runs over, the one named last changes fastest.
Arguments:
- tokens: bfloat16 [4, 2048, 2048], P(('grp', 'fs'), ('sp', 'tp')), parts along dimension 0, may hold values from -6 to 6
- norm_gain: float32 [2048], replicated, may hold values from 0.1 to 1.9
- w_bgate: bfloat16 [2048, 2048], P(('sp', 'fs'), 'tp'), may hold values from -0.125 to 0.125
- w_cgate: bfloat16 [2048, 2048], P(('sp', 'fs'), 'tp'), may hold values from -0.125 to 0.125
- w_conv_in: bfloat16 [2048, 2048], P(('sp', 'fs'), 'tp'), may hold values from -0.125 to 0.125
- conv_taps: bfloat16 [3, 2048], P(None, 'tp'), may hold values from -3.5 to 3.5
- w_query: bfloat16 [2048, 2048], P(('sp', 'fs'), 'tp'), may hold values from -0.13258252 to 0.13258252
- w_key: bfloat16 [2048, 256], P(('sp', 'fs'), 'tp'), may hold values from -4.02167 to 4.02167
- w_value: bfloat16 [2048, 256], P(('sp', 'fs'), 'tp'), may hold values from -0.125 to 0.125
- sink_logits: float32 [32], P('tp'), may hold values from 1 to 6
- conv_out_weight: bfloat16 [2048, 2048], P('tp', ('sp', 'fs')), may hold values from -0.125 to 0.125
- attn_out_weight: bfloat16 [2048, 2048], P('tp', ('sp', 'fs')), may hold values from -0.75 to 0.75
Outputs:
- mixed: bfloat16 [4, 2048, 2048], P(('grp', 'fs'), ('sp', 'tp')), parts along dimension 0
The draws below stay inside these ranges and needn't reach their ends.
There are 2 independent parts, one for each index of `grp`. The reference program is written for one: setup_inputs(seed, part) draws one part's arguments, and reference() takes and returns one part's arrays. A program takes and returns all parts, laid end to end along the dimension named above; an argument that names none is the same for every part. Nothing has to cross between parts.
All inputs are finite; a program needn't handle non-finite values.
Results may differ from the reference program's by a relative error of at most 0.014.
The reference program's roundings to bfloat16 on the way count: a program that leaves them out, or rounds other values in their place, can miss the bound.
Values may be sent and summed in bfloat16 or wider, within the bound.
A program may use at most 128 MiB of HBM per device.

```python
import jax
import jax.numpy as jnp
from jax import lax

D = 2048
CONV = 2048
HEADS = 32
KV_HEADS = 4
HEAD = 64
WINDOW = 128
TAPS = 3
ATTN_Q = 2048
ATTN_KV = 256
SEQS = 2
LENGTH = 2048
N_TP = 2


def query_matrix(key):
    raw = jax.random.normal(jax.random.fold_in(key, 31), (D, ATTN_Q), jnp.float32)
    return jnp.clip(raw, -6.0, 6.0) / jnp.sqrt(jnp.float32(D))


def draw_w_query(key, part):
    return query_matrix(key).astype(jnp.bfloat16)


def draw_w_key(key, part):
    raw = jax.random.normal(jax.random.fold_in(key, 32), (D, ATTN_KV), jnp.float32)
    noise = jnp.clip(raw, -6.0, 6.0) / jnp.sqrt(jnp.float32(D))
    return noise.astype(jnp.bfloat16)


def draw_tokens(key, part):
    base = jnp.clip(jax.random.normal(jax.random.fold_in(key, 41), (SEQS, LENGTH, D), jnp.float32), -6.0, 6.0)
    return base.astype(jnp.bfloat16)


def steps_of(rng, shape, shards, smallest, high):
    gain = 1.0
    for dim, parts in shards:
        draws = jax.random.uniform(jax.random.fold_in(jax.random.fold_in(rng, 6), dim), (parts,), jnp.float32, smallest / len(shards), high / len(shards))
        gain = gain * jnp.repeat(jnp.exp(draws), shape[dim] // parts).reshape((-1,) + (1,) * (len(shape) - 1 - dim))
    return gain


def normal_values(own_key, shape, spread, bound, pieces=(), kind=jnp.bfloat16):
    array = jax.random.normal(own_key, shape, jnp.float32) * spread
    if len(pieces) > 0:
        array = steps_of(own_key, shape, pieces, -0.22, 0.18) * array
    return jnp.clip(array, min=-bound, max=bound).astype(kind)


def setup_inputs(seed: int = 0, part: int = 0) -> dict:
    key_list = jax.random.split(jax.random.key(seed), 13)
    own_keys = jax.random.split(jax.random.fold_in(key_list[12], part), 13)
    return {
        "tokens": draw_tokens(jax.random.fold_in(jax.random.fold_in(key_list[12], part), 71), part),
        "norm_gain": jnp.clip(1.0 + 0.18 * jax.random.normal(key_list[1], (D,), jnp.float32), 0.1, 1.9),
        "w_bgate": normal_values(key_list[2], (D, CONV), D ** -0.5, 0.125, ((0, 8), (1, 2))),
        "w_cgate": normal_values(key_list[3], (D, CONV), D ** -0.5, 0.125, ((0, 8), (1, 2))),
        "w_conv_in": normal_values(key_list[4], (D, CONV), D ** -0.5, 0.125, ((0, 8), (1, 2))),
        "conv_taps": normal_values(key_list[5], (TAPS, CONV), TAPS ** -0.5, 3.5, ((1, 2),)),
        "w_query": draw_w_query(jax.random.fold_in(key_list[12], 71), part),
        "w_key": draw_w_key(jax.random.fold_in(key_list[12], 71), part),
        "w_value": normal_values(key_list[8], (D, ATTN_KV), D ** -0.5, 0.125, ((0, 8), (1, 2))),
        "sink_logits": jnp.clip(1.0 + 5.0 * jax.random.uniform(key_list[9], (HEADS,), jnp.float32) ** steps_of(key_list[9], (HEADS,), ((0, 2),), -0.2, 0.2), 1.0, 6.0),
        "conv_out_weight": normal_values(key_list[10], (CONV, D), CONV ** -0.5, 0.125, ((0, 2), (1, 8))),
        "attn_out_weight": normal_values(key_list[11], (ATTN_Q, D), (ATTN_Q // 32) ** -0.5, 0.75, ((0, 2), (1, 8))),
    }


epsilon = 1e-06

def window_attention(queries, key_rows, value_rows, sink_logits):
    length = queries.shape[0]
    blocks = length // WINDOW
    groups = HEADS // KV_HEADS
    query_blocks = queries.astype(jnp.float32).reshape(blocks, WINDOW, KV_HEADS, groups, HEAD)
    zero_rows = jnp.zeros((WINDOW, ATTN_KV), jnp.float32)
    key_all = jnp.concatenate([zero_rows, key_rows.astype(jnp.float32)], 0)
    value_all = jnp.concatenate([zero_rows, value_rows.astype(jnp.float32)], 0)
    key_band = jnp.concatenate([key_all[:length].reshape(blocks, WINDOW, KV_HEADS, HEAD), key_all[WINDOW:].reshape(blocks, WINDOW, KV_HEADS, HEAD)], 1)
    value_band = jnp.concatenate([value_all[:length].reshape(blocks, WINDOW, KV_HEADS, HEAD), value_all[WINDOW:].reshape(blocks, WINDOW, KV_HEADS, HEAD)], 1)
    scores = jnp.einsum('nqhgd,nkhd->nhgqk', query_blocks, key_band) / jnp.sqrt(jnp.float32(HEAD))
    block_ids = jnp.arange(blocks)[:, None, None]
    query_pos = block_ids * WINDOW + jnp.arange(WINDOW)[None, :, None]
    key_pos = (block_ids - 1) * WINDOW + jnp.arange(2 * WINDOW)[None, None, :]
    allowed = (key_pos >= 0) & (key_pos <= query_pos) & (query_pos - key_pos < WINDOW)
    scores = jnp.where(allowed[:, None, None], scores, -jnp.inf)
    sink_grid = sink_logits.astype(jnp.float32).reshape(1, KV_HEADS, groups, 1, 1)
    peak_score = jnp.maximum(lax.optimization_barrier(jnp.max(scores, axis=-1, keepdims=True)), sink_grid)
    weights = jnp.exp(scores - peak_score)
    denominator = lax.optimization_barrier(jnp.sum(weights, axis=-1, keepdims=True)) + jnp.exp(sink_grid - peak_score)
    probabilities = (weights / denominator).astype(jnp.bfloat16)
    attended = jnp.einsum('nhgqk,nkhd->nqhgd', probabilities.astype(jnp.float32), value_band)
    return attended.astype(jnp.bfloat16).reshape(length, ATTN_Q)

def one_sequence(tokens, norm_gain, w_bgate, w_cgate, w_conv_in, conv_taps, w_query, w_key, w_value, sink_logits, conv_out_weight, attn_out_weight):
    widened = tokens.astype(jnp.float32)
    normed = (widened * lax.rsqrt(lax.optimization_barrier(jnp.mean(widened * widened, axis=-1, keepdims=True)) + epsilon) * norm_gain).astype(jnp.bfloat16)

    def project(weight):
        return jnp.dot(normed, weight, preferred_element_type=jnp.float32).astype(jnp.bfloat16)
    out_gate = project(w_bgate)
    in_gate = project(w_cgate)
    conv_input = project(w_conv_in)
    queries = project(w_query)
    key_rows = project(w_key)
    value_rows = project(w_value)
    length = tokens.shape[0]
    gated = (in_gate.astype(jnp.float32) * conv_input.astype(jnp.float32)).astype(jnp.bfloat16)
    padded = jnp.concatenate([jnp.zeros((TAPS - 1, CONV), jnp.bfloat16), gated], 0)
    taps_wide = conv_taps.astype(jnp.float32)
    convolved = padded[0:length].astype(jnp.float32) * taps_wide[0]
    for which in range(1, TAPS):
        convolved = convolved + padded[which:which + length].astype(jnp.float32) * taps_wide[which]
    conv_branch = (out_gate.astype(jnp.float32) * convolved).astype(jnp.bfloat16)
    attended = window_attention(queries, key_rows, value_rows, sink_logits)
    conv_parts = conv_branch.reshape(length, N_TP, CONV // N_TP)
    attn_parts = attended.reshape(length, N_TP, ATTN_Q // N_TP)
    conv_weight_parts = conv_out_weight.reshape(N_TP, CONV // N_TP, D)
    attn_weight_parts = attn_out_weight.reshape(N_TP, ATTN_Q // N_TP, D)
    running = jnp.zeros((length, D), jnp.float32)
    for member in range(N_TP):
        partial_value = jnp.dot(conv_parts[:, member], conv_weight_parts[member], preferred_element_type=jnp.float32)
        partial_value = partial_value + jnp.dot(attn_parts[:, member], attn_weight_parts[member], preferred_element_type=jnp.float32)
        rounded = lax.optimization_barrier(partial_value.astype(jnp.bfloat16))
        running = running + rounded.astype(jnp.float32)
    return running.astype(jnp.bfloat16)

def reference(tokens, norm_gain, w_bgate, w_cgate, w_conv_in, conv_taps, w_query, w_key, w_value, sink_logits, conv_out_weight, attn_out_weight):
    results = []
    for sequence in range(SEQS):
        results.append(one_sequence(tokens[sequence], norm_gain, w_bgate, w_cgate, w_conv_in, conv_taps, w_query, w_key, w_value, sink_logits, conv_out_weight, attn_out_weight))
    return jnp.stack(results, 0)
```

```python
import functools

import jax
import jax.numpy as jnp
from jax import lax
from jax.experimental import pallas as pl
from jax.experimental.pallas import tpu as pltpu
from jax.sharding import PartitionSpec as P

HEAD = 64
WINDOW = 128
TAPS = 3
LANES = 128
HALO = 16
TILE = 256
MESH = pl.DeviceIdType.MESH

epsilon = 1e-06


def spans(kv, conv):
    third = conv * 3 // 8 // LANES * LANES
    arrays = [(0, 2 * kv, kv)]
    for which in range(6):
        arrays.append((2 * kv + which * conv, conv, third))
    return arrays


def kernel(
    sizes,
    normed,
    packed,
    taps,
    sink,
    out,
    weights,
    rows,
    query,
    keys,
    gate,
    gated,
    conv,
    attended,
    partial,
    theirs,
    local_sem,
    pair_sem,
    halo_sem,
    z_send,
    x_send,
    y_send,
    zx_recv,
    y_recv,
    swap_send,
    swap_recv,
):
    n, m, own, kv, width = sizes
    depth = weights.shape[1]
    features = rows.shape[1]
    length = 2 * own
    grp, sp = lax.axis_index("grp"), lax.axis_index("sp")
    fs, tp = lax.axis_index("fs"), lax.axis_index("tp")
    arrays = spans(kv, width)
    mine = sp * m + fs

    barrier = pltpu.get_barrier_semaphore()

    def greet(axis, device):
        pl.semaphore_signal(barrier, inc=1, device_id={axis: device}, device_id_type=MESH)

    fill = pltpu.make_async_copy(packed, weights.at[mine], local_sem.at[0])
    fill.start()
    at_own = pl.multiple_of(WINDOW + tp * own, LANES)
    place = pltpu.make_async_copy(normed, rows.at[pl.ds(at_own, own)], local_sem.at[1])
    place.start()

    def greet_sp(d, _):
        greet("sp", lax.rem(sp + d, n))
        return _

    def greet_fs(d, _):
        greet("fs", lax.rem(fs + d, m))
        return _

    lax.fori_loop(1, n, greet_sp, 0)
    lax.fori_loop(1, m, greet_fs, 0)
    greet("grp", 1 - grp)
    greet("tp", 1 - tp)
    pl.semaphore_wait(barrier, n + m)

    sibling = pltpu.make_async_remote_copy(
        normed,
        rows.at[pl.ds(at_own, own)],
        pair_sem.at[0],
        pair_sem.at[1],
        device_id={"tp": 1 - tp},
        device_id_type=MESH,
    )
    sibling.start()

    def halo_copy(source, where):
        return pltpu.make_async_remote_copy(
            source,
            rows.at[pl.ds(0, WINDOW)],
            halo_sem.at[0],
            halo_sem.at[1],
            device_id=where,
            device_id_type=MESH,
        )

    onward = halo_copy(normed.at[pl.ds(own - WINDOW, WINDOW)], {"sp": lax.rem(sp + 1, n)})
    across = pltpu.make_async_remote_copy(
        rows.at[pl.ds(0, WINDOW)],
        rows.at[pl.ds(0, WINDOW)],
        halo_sem.at[2],
        halo_sem.at[1],
        device_id={"tp": 1 - tp},
        device_id_type=MESH,
    )

    @pl.when((tp == 1) & (sp < n - 1))
    def _():
        onward.start()

    @pl.when(sp == 0)
    def _():
        rows[pl.ds(0, WINDOW), :] = jnp.zeros((WINDOW, features), jnp.bfloat16)

    fill.wait()

    def fetched(j):
        first, total, alone = arrays[j]
        return pl.ds(pl.multiple_of(first + grp * alone, LANES), total - alone)

    def lone(j, group):
        first, total, alone = arrays[j]
        return pl.ds(pl.multiple_of(first + group * (total - alone), LANES), alone)

    def along_z(j, d, chunk):
        piece = weights.at[chunk, :, fetched(j)]
        return pltpu.make_async_remote_copy(
            piece,
            piece,
            z_send.at[j, d],
            zx_recv.at[j, chunk],
            device_id={"sp": lax.rem(sp + d, n)},
            device_id_type=MESH,
        )

    def along_x(j, s, d, chunk):
        piece = weights.at[chunk, :, fetched(j)]
        return pltpu.make_async_remote_copy(
            piece,
            piece,
            x_send.at[j, s, d],
            zx_recv.at[j, chunk],
            device_id={"fs": lax.rem(fs + d, m)},
            device_id_type=MESH,
        )

    def along_y(j, chunk, group):
        piece = weights.at[chunk, :, lone(j, group)]
        return pltpu.make_async_remote_copy(
            piece,
            piece,
            y_send.at[j, chunk],
            y_recv.at[j, chunk],
            device_id={"grp": 1 - grp},
            device_id_type=MESH,
        )

    def loop(low, high, body):
        def step(i, carry):
            body(i)
            return carry

        lax.fori_loop(low, high, step, 0)

    def open_links(j):
        loop(1, n, lambda d: along_z(j, d, mine).start())
        loop(1, m, lambda d: along_x(j, sp, d, mine).start())

    def from_z(j):
        def body(d):
            s = lax.rem(sp + d, n)
            chunk = s * m + fs
            along_z(j, d, chunk).wait_recv()
            loop(1, m, lambda e: along_x(j, s, e, chunk).start())
            along_y(j, chunk, grp).start()

        loop(1, n, body)

    def from_x(j):
        def body(d):
            s = lax.rem(sp + d, n)

            def inner(e):
                chunk = s * m + lax.rem(fs + e, m)
                along_x(j, s, e, chunk).wait_recv()
                along_y(j, chunk, grp).start()

            loop(1, m, inner)

        loop(0, n, body)

    def from_y(j):
        def body(d):
            chunk = lax.rem(mine + d, n * m)
            along_y(j, chunk, 1 - grp).wait_recv()

        loop(1, n * m, body)

    for j in range(len(arrays)):
        open_links(j)

    place.wait()
    sibling.wait()

    @pl.when((tp == 1) & (sp > 0))
    def _():
        onward.wait_recv()
        across.start()

    @pl.when((tp == 0) & (sp > 0))
    def _():
        across.wait_recv()

    def project(first, low, count, columns):
        block = weights[:, :, pl.ds(first, columns)].reshape(n * m * depth, columns)
        return jnp.dot(
            rows[pl.ds(low, count), :], block, preferred_element_type=jnp.float32
        ).astype(jnp.bfloat16)

    def tiles(total, body):
        step = min(TILE, total)
        loop(0, total // step, lambda t: body(pl.multiple_of(t * step, LANES), step))

    def do_keys():
        keys[...] = project(0, 0, WINDOW + length, 2 * kv)

    def do_query():
        def body(at, step):
            query[:, pl.ds(at, step)] = project(arrays[1][0] + at, WINDOW, length, step)

        tiles(width, body)

    def do_attention():
        pairs = 2 * HEAD
        per_kv = width // kv
        blocks = length // WINDOW
        place_q = lax.broadcasted_iota(jnp.int32, (WINDOW, 2 * WINDOW), 0)
        place_k = lax.broadcasted_iota(jnp.int32, (WINDOW, 2 * WINDOW), 1)
        banded = (place_k > place_q) & (place_k <= place_q + WINDOW)
        for head in range(kv // HEAD):

            def body(i):
                b = i // (per_kv // 2)
                p = lax.rem(i, per_kv // 2)
                at = pl.multiple_of((head * (per_kv // 2) + p) * pairs, LANES)
                row = pl.multiple_of(b * WINDOW, WINDOW)
                band = keys[pl.ds(row, 2 * WINDOW), :]
                key = band[:, head * HEAD : (head + 1) * HEAD]
                value = band[:, kv + head * HEAD : kv + (head + 1) * HEAD]
                least = jnp.where((sp == 0) & (b == 0), WINDOW, 0)
                allowed = banded & (place_k >= least)
                both = query[pl.ds(row, WINDOW), pl.ds(at, pairs)]
                results = []
                for half in range(2):
                    one = both[:, half * HEAD : (half + 1) * HEAD]
                    scores = lax.dot_general(
                        one, key, (((1,), (1,)), ((), ())), preferred_element_type=jnp.float32
                    ) * (1.0 / HEAD**0.5)
                    scores = jnp.where(allowed, scores, -jnp.inf)
                    logit = sink[head * per_kv + 2 * p + half]
                    peak = jnp.maximum(jnp.max(scores, axis=-1, keepdims=True), logit)
                    powers = jnp.exp(scores - peak)
                    total = jnp.sum(powers, axis=-1, keepdims=True) + jnp.exp(logit - peak)
                    probs = (powers / total).astype(jnp.bfloat16)
                    results.append(jnp.dot(probs, value, preferred_element_type=jnp.float32))
                attended[pl.ds(row, WINDOW), pl.ds(at, pairs)] = jnp.concatenate(
                    results, axis=1
                ).astype(jnp.bfloat16)

            loop(0, blocks * (per_kv // 2), body)

    def do_gate():
        def body(at, step):
            gate[:, pl.ds(at, step)] = project(
                arrays[2][0] + at, WINDOW - HALO, HALO + length, step
            )

        tiles(width, body)

    def do_gated():
        def body(at, step):
            values = project(arrays[3][0] + at, WINDOW - HALO, HALO + length, step)
            product = gate[:, pl.ds(at, step)].astype(jnp.float32) * values.astype(jnp.float32)
            gated[:, pl.ds(at, step)] = product.astype(jnp.bfloat16).astype(jnp.float32)

        tiles(width, body)

    def do_conv():
        def body(at, step):
            outer = project(arrays[4][0] + at, WINDOW, length, step).astype(jnp.float32)
            mixed = None
            for which in range(TAPS):
                tap = taps[pl.ds(which, 1), pl.ds(at, step)].astype(jnp.float32)
                term = tap * gated[pl.ds(HALO - TAPS + 1 + which, length), pl.ds(at, step)]
                mixed = term if mixed is None else mixed + term
            conv[:, pl.ds(at, step)] = (outer * mixed).astype(jnp.bfloat16)

        tiles(width, body)

    work = [do_keys, do_query, do_gate, do_gated, do_conv, None, None]
    count = len(arrays)
    for step in range(count + 2):
        if step < count:
            from_z(step)
        if 0 <= step - 1 < count:
            from_x(step - 1)
        if step >= 2:
            from_y(step - 2)
            if work[step - 2] is not None:
                work[step - 2]()
            if step == 4:
                do_attention()

    def swap(t, step):
        piece = pl.ds(pl.multiple_of(t * step, LANES), step)
        return pltpu.make_async_remote_copy(
            partial.at[1, :, piece],
            theirs.at[:, piece],
            swap_send.at[t],
            swap_recv.at[t],
            device_id={"tp": 1 - tp},
            device_id_type=MESH,
        )

    step = depth
    per = max(1, TILE // depth)
    step = per * depth
    count_out = n * m // per

    def share(low, t):
        total = None
        for j, left in ((5, conv), (6, attended)):
            block = weights[pl.ds(t * per, per), :, pl.ds(arrays[j][0], width)]
            term = lax.dot_general(
                left[pl.ds(low, own), :],
                block.reshape(step, width),
                (((1,), (1,)), ((), ())),
                preferred_element_type=jnp.float32,
            )
            total = term if total is None else total + term
        return total.astype(jnp.bfloat16)

    def final(t):
        piece = pl.ds(pl.multiple_of(t * step, LANES), step)
        partial[1, :, piece] = share(pl.multiple_of((1 - tp) * own, LANES), t)
        partial[0, :, piece] = share(pl.multiple_of(tp * own, LANES), t)
        swap(t, step).start()

    loop(0, count_out, final)

    def add(t):
        piece = pl.ds(pl.multiple_of(t * step, LANES), step)
        swap(t, step).wait()
        out[:, piece] = (
            partial[0, :, piece].astype(jnp.float32) + theirs[:, piece].astype(jnp.float32)
        ).astype(jnp.bfloat16)

    loop(0, count_out, add)

    for j in range(count):
        loop(1, n, lambda d: along_z(j, d, mine).wait_send())

        def x_done(d):
            s = lax.rem(sp + d, n)
            loop(1, m, lambda e: along_x(j, s, e, s * m + fs).wait_send())

        loop(0, n, x_done)
        loop(1, n * m, lambda d: along_y(j, lax.rem(mine + d, n * m), grp).wait_send())

    @pl.when((tp == 1) & (sp < n - 1))
    def _():
        onward.wait_send()

    @pl.when((tp == 1) & (sp > 0))
    def _():
        across.wait_send()


def local(
    n,
    m,
    tokens,
    norm_gain,
    w_bgate,
    w_cgate,
    w_conv_in,
    conv_taps,
    w_query,
    w_key,
    w_value,
    sink_logits,
    conv_out_weight,
    attn_out_weight,
):
    widened = tokens[0].astype(jnp.float32)
    normed = (
        widened
        * lax.rsqrt(jnp.mean(widened * widened, axis=-1, keepdims=True) + epsilon)
        * norm_gain
    ).astype(jnp.bfloat16)
    packed = jnp.concatenate(
        [
            w_key,
            w_value,
            w_query,
            w_cgate,
            w_conv_in,
            w_bgate,
            conv_out_weight.T,
            attn_out_weight.T,
        ],
        1,
    )
    own, features = normed.shape
    length = 2 * own
    kv, width = w_key.shape[1], w_query.shape[1]
    depth = packed.shape[0]
    arrays = len(spans(kv, width))
    chunks = n * m
    bf16 = jnp.bfloat16
    vmem = pl.BlockSpec(memory_space=pltpu.VMEM)
    whole = pl.BlockSpec(memory_space=pl.ANY)
    dma = pltpu.SemaphoreType.DMA
    mixed = pl.pallas_call(
        functools.partial(kernel, (n, m, own, kv, width)),
        out_shape=jax.ShapeDtypeStruct((own, features), bf16),
        in_specs=[whole, whole, vmem, pl.BlockSpec(memory_space=pltpu.SMEM)],
        out_specs=vmem,
        scratch_shapes=[
            pltpu.VMEM((chunks,) + packed.shape, bf16),
            pltpu.VMEM((WINDOW + length, features), bf16),
            pltpu.VMEM((length, width), bf16),
            pltpu.VMEM((WINDOW + length, 2 * kv), bf16),
            pltpu.VMEM((HALO + length, width), bf16),
            pltpu.VMEM((HALO + length, width), jnp.float32),
            pltpu.VMEM((length, width), bf16),
            pltpu.VMEM((length, width), bf16),
            pltpu.VMEM((2, own, features), bf16),
            pltpu.VMEM((own, features), bf16),
            dma((2,)),
            dma((2,)),
            dma((3,)),
            dma((arrays, n)),
            dma((arrays, n, m)),
            dma((arrays, chunks)),
            dma((arrays, chunks)),
            dma((arrays, chunks)),
            dma((chunks,)),
            dma((chunks,)),
        ],
        compiler_params=pltpu.CompilerParams(
            collective_id=0, has_side_effects=True, vmem_limit_bytes=64_000_000
        ),
    )(normed, packed, conv_taps, sink_logits)
    return mixed[None]


def solution(mesh):
    placed = (
        P(("grp", "fs"), ("sp", "tp"), None),
        P(),
        P(("sp", "fs"), "tp"),
        P(("sp", "fs"), "tp"),
        P(("sp", "fs"), "tp"),
        P(None, "tp"),
        P(("sp", "fs"), "tp"),
        P(("sp", "fs"), "tp"),
        P(("sp", "fs"), "tp"),
        P("tp"),
        P("tp", ("sp", "fs")),
        P("tp", ("sp", "fs")),
    )
    return jax.shard_map(
        functools.partial(local, mesh.shape["sp"], mesh.shape["fs"]),
        mesh=mesh,
        in_specs=placed,
        out_specs=P(("grp", "fs"), ("sp", "tp"), None),
        check_vma=False,
    )
```

```python
import functools

import jax
import jax.numpy as jnp
from jax import lax
from jax.experimental import pallas as pl
from jax.experimental.pallas import tpu as pltpu
from jax.sharding import PartitionSpec as P

HEAD = 64
WINDOW = 128
TAPS = 3
LANES = 128
HALO = 16
TILE = 256
UNIT = 16
MESH = pl.DeviceIdType.MESH

epsilon = 1e-06


def part(count, eighths):
    return max(UNIT, count * eighths // 8 // UNIT * UNIT)


def kernel(
    n,
    m,
    normed,
    w_key,
    w_value,
    w_query,
    w_cgate,
    w_conv_in,
    w_bgate,
    conv_weight,
    attn_weight,
    taps,
    sink,
    out,
    w_in,
    w_out,
    rows,
    query,
    keys,
    gate,
    mine_conv,
    conv,
    attended,
    total,
    partial,
    theirs,
    local_sem,
    rows_send,
    rows_recv,
    halo_send,
    halo_recv,
    trade_send,
    trade_recv,
    in_send,
    in_recv,
    in_y_send,
    in_y_recv,
    z_send,
    x_send,
    out_recv,
    y_send,
    y_recv,
    give_send,
    give_recv,
    swap_send,
    swap_recv,
):
    inputs = (w_key, w_value, w_query, w_cgate, w_conv_in, w_bgate)
    outputs = (conv_weight, attn_weight)
    own, features = normed.shape
    length = 2 * own
    span = WINDOW + length
    depth, kv = w_key.shape
    width = w_query.shape[1]
    slim = width // m
    across_out = conv_weight.shape[1]
    heads = slim // HEAD
    per_kv = width // kv
    chunks = n * m
    firsts = [0, kv] + [2 * kv + i * slim for i in range(4)]
    sizes = [kv, kv] + [slim] * 4
    in_alone = [part(depth, 4)] * 6
    out_alone = [part(width, 4), part(width, 3)]

    grp, sp = lax.axis_index("grp"), lax.axis_index("sp")
    fs, tp = lax.axis_index("fs"), lax.axis_index("tp")
    mine = sp * m + fs

    def loop(low, high, body):
        def step(i, carry):
            body(i)
            return carry

        lax.fori_loop(low, high, step, 0)

    def remote(source, target, send, recv, where):
        return pltpu.make_async_remote_copy(
            source, target, send, recv, device_id=where, device_id_type=MESH
        )

    def to_sp(d):
        return {"sp": lax.rem(sp + d, n)}

    def to_fs(e):
        return {"fs": lax.rem(fs + e, m)}

    other_core = {"tp": 1 - tp}
    other_grp = {"grp": 1 - grp}

    def columns(j, f):
        if j < 2:
            return pl.ds(0, kv)
        return pl.ds(pl.multiple_of(f * slim, LANES), slim)

    def kept(j):
        return pl.ds(firsts[j], sizes[j])

    fills = [
        pltpu.make_async_copy(
            inputs[j].at[:, columns(j, fs)], w_in.at[mine, :, kept(j)], local_sem.at[j]
        )
        for j in range(6)
    ] + [
        pltpu.make_async_copy(outputs[j], w_out.at[j, mine], local_sem.at[6 + j]) for j in range(2)
    ]
    at_own = pl.multiple_of(WINDOW + tp * own, LANES)
    at_other = pl.multiple_of(WINDOW + (1 - tp) * own, LANES)
    fills.append(
        pltpu.make_async_copy(normed, rows.at[fs, pl.ds(at_own, own)], local_sem.at[8])
    )
    for fill in fills:
        fill.start()

    @pl.when(sp == 0)
    def _():
        for i in range(m):
            rows[i, pl.ds(0, WINDOW), :] = jnp.zeros((WINDOW, features), jnp.bfloat16)

    barrier = pltpu.get_barrier_semaphore()

    def greet(where):
        pl.semaphore_signal(barrier, inc=1, device_id=where, device_id_type=MESH)

    loop(1, n, lambda d: greet(to_sp(d)))
    loop(1, m, lambda e: greet(to_fs(e)))
    greet(other_grp)
    greet(other_core)
    pl.semaphore_wait(barrier, n + m)

    def trade(j, e):
        f = lax.rem(fs + e, m)
        return remote(
            inputs[j].at[:, columns(j, f)],
            w_in.at[mine, :, kept(j)],
            trade_send.at[j, e],
            trade_recv.at[j, fs],
            {"fs": f},
        )

    def trade_arrival(j, f):
        piece = w_in.at[sp * m + f, :, kept(j)]
        return remote(piece, piece, trade_send.at[j, 0], trade_recv.at[j, f], to_fs(1))

    def in_rows(j):
        return pl.ds(pl.multiple_of(grp * in_alone[j], UNIT), depth - in_alone[j])

    def in_lone(j, group):
        return pl.ds(
            pl.multiple_of(group * (depth - in_alone[j]), UNIT), in_alone[j]
        )

    def in_z(j, d, chunk, f):
        piece = w_in.at[chunk, in_rows(j), kept(j)]
        return remote(piece, piece, in_send.at[j, d, f], in_recv.at[j, chunk], to_sp(d))

    def in_y(j, chunk, group):
        piece = w_in.at[chunk, in_lone(j, group), kept(j)]
        return remote(piece, piece, in_y_send.at[j, chunk], in_y_recv.at[j, chunk], other_grp)

    def rows_copy(source, f, core, send, where):
        at = pl.multiple_of(WINDOW + core * own, LANES)
        return remote(
            source, rows.at[f, pl.ds(at, own)], rows_send.at[send], rows_recv.at[f, core], where
        )

    def rows_x(e):
        return rows_copy(normed, fs, tp, e, to_fs(e))

    def rows_core(f):
        return rows_copy(rows.at[f, pl.ds(at_own, own)], f, tp, m + f, other_core)

    def halo_copy(source, f, send, where):
        return remote(
            source, rows.at[f, pl.ds(0, WINDOW)], halo_send.at[send], halo_recv.at[f], where
        )

    def halo_here(f):
        return rows.at[f, pl.ds(0, WINDOW)]

    onward = halo_copy(normed.at[pl.ds(own - WINDOW, WINDOW)], fs, 0, to_sp(1))

    def out_rows(j):
        return pl.ds(pl.multiple_of(grp * out_alone[j], UNIT), width - out_alone[j])

    def out_lone(j, group):
        return pl.ds(pl.multiple_of(group * (width - out_alone[j]), UNIT), out_alone[j])

    def along_z(j, d):
        piece = w_out.at[j, mine, out_rows(j)]
        return remote(piece, piece, z_send.at[j, d], out_recv.at[j, mine], to_sp(d))

    def along_x(j, s, e, chunk):
        piece = w_out.at[j, chunk, out_rows(j)]
        return remote(piece, piece, x_send.at[j, s, e], out_recv.at[j, chunk], to_fs(e))

    def arrival(j, chunk):
        piece = w_out.at[j, chunk, out_rows(j)]
        return remote(piece, piece, z_send.at[j, 0], out_recv.at[j, chunk], to_sp(1))

    def along_y(j, chunk, group):
        piece = w_out.at[j, chunk, out_lone(j, group)]
        return remote(piece, piece, y_send.at[j, chunk], y_recv.at[j, chunk], other_grp)

    for j in range(6):
        loop(1, m, lambda e: trade(j, e).start())
        if j == 1:

            @pl.when((tp == 1) & (sp < n - 1))
            def _():
                onward.start()

    loop(1, m, lambda e: rows_x(e).start())
    for j in range(6):
        fills[j].wait()
        loop(1, n, lambda d: in_z(j, d, mine, fs).start())
    fills[8].wait()
    rows_core(fs).start()
    for j in range(6):

        def traded(e):
            f = lax.rem(fs + e, m)
            trade_arrival(j, f).wait_recv()
            loop(1, n, lambda d: in_z(j, d, sp * m + f, f).start())

        loop(1, m, traded)
    for j in range(2):
        fills[6 + j].wait()
        loop(1, n, lambda d: along_z(j, d).start())
        loop(1, m, lambda e: along_x(j, sp, e, mine).start())

    def rows_on(e):
        f = lax.rem(fs + e, m)
        rows_copy(rows.at[f, pl.ds(at_own, own)], f, tp, 0, to_fs(e)).wait_recv()
        rows_core(f).start()

    loop(1, m, rows_on)

    @pl.when((tp == 1) & (sp > 0))
    def _():
        halo_copy(halo_here(fs), fs, 0, other_core).wait_recv()
        halo_copy(halo_here(fs), fs, 1 + fs, other_core).start()
        loop(1, m, lambda e: halo_copy(halo_here(fs), fs, m + e, to_fs(e)).start())

        def pass_on(e):
            f = lax.rem(fs + e, m)
            halo_copy(halo_here(f), f, 0, other_core).wait_recv()
            halo_copy(halo_here(f), f, 1 + f, other_core).start()

        loop(1, m, pass_on)

    def rows_in(f):
        piece = rows.at[f, pl.ds(at_other, own)]
        remote(piece, piece, rows_send.at[0], rows_recv.at[f, 1 - tp], other_core).wait_recv()

    loop(0, m, rows_in)

    @pl.when((tp == 0) & (sp > 0))
    def _():
        loop(0, m, lambda f: halo_copy(halo_here(f), f, 0, other_core).wait_recv())

    def in_from_z(j):
        def body(i):
            s = lax.rem(sp + 1 + i // m, n)
            chunk = s * m + lax.rem(fs + i, m)
            in_z(j, 1, chunk, fs).wait_recv()
            in_y(j, chunk, grp).start()

        loop(0, (n - 1) * m, body)

    def in_from_y(j):
        def body(i):
            s = lax.rem(sp + 1 + i // m, n)
            in_y(j, s * m + lax.rem(fs + i, m), 1 - grp).wait_recv()

        loop(0, (n - 1) * m, body)

    def from_z(j):
        def body(d):
            s = lax.rem(sp + d, n)
            chunk = s * m + fs
            arrival(j, chunk).wait_recv()
            loop(1, m, lambda e: along_x(j, s, e, chunk).start())
            along_y(j, chunk, grp).start()

        loop(1, n, body)

    def from_x(j):
        def body(d):
            s = lax.rem(sp + d, n)

            def inner(e):
                chunk = s * m + lax.rem(fs + e, m)
                arrival(j, chunk).wait_recv()
                along_y(j, chunk, grp).start()

            loop(1, m, inner)

        loop(0, n, body)

    def from_y(j):
        loop(
            1,
            chunks,
            lambda d: along_y(j, lax.rem(mine + d, chunks), 1 - grp).wait_recv(),
        )

    def project(i, first, count):
        block = w_in[:, :, pl.ds(first, count)].reshape(chunks * depth, count)
        return jnp.dot(rows[i], block, preferred_element_type=jnp.float32).astype(jnp.bfloat16)

    def tiles(body):
        step = min(TILE, slim)
        for i in range(m):
            loop(0, slim // step, lambda t: body(i, pl.multiple_of(t * step, LANES), step))

    kv_head = fs * heads // per_kv

    def do_keys():
        for i in range(m):
            both = project(i, 0, 2 * kv).astype(jnp.float32)
            picked = []
            for base in (0, kv):
                one = both[:, base : base + HEAD]
                for h in range(1, kv // HEAD):
                    at = base + h * HEAD
                    one = jnp.where(kv_head == h, both[:, at : at + HEAD], one)
                picked.append(one)
            keys[i] = jnp.concatenate(picked, axis=1).astype(jnp.bfloat16)

    def do_query():
        def body(i, at, step):
            query[i, :, pl.ds(at, step)] = project(i, firsts[2] + at, step)

        tiles(body)

    def result(which, f):
        return mine_conv.at[f] if which == 0 else query.at[f, pl.ds(WINDOW, length)]

    def give(which, e):
        full = (conv, attended)[which]
        f = lax.rem(fs + e, m)
        here = pl.ds(pl.multiple_of(fs * slim, LANES), slim)
        return remote(
            result(which, f), full.at[:, here], give_send.at[which, e], give_recv.at[which, fs], {"fs": f}
        )

    def given(which, e):
        full = (conv, attended)[which]
        f = lax.rem(fs + e, m)
        piece = full.at[:, pl.ds(pl.multiple_of(f * slim, LANES), slim)]
        return remote(piece, piece, give_send.at[which, 0], give_recv.at[which, f], to_fs(e))

    def keep(which):
        full = (conv, attended)[which]
        full[:, pl.ds(pl.multiple_of(fs * slim, LANES), slim)] = result(which, fs)[...]

    def do_attention():
        pairs = 2 * HEAD
        blocks = length // WINDOW
        count = heads // 2
        place_q = lax.broadcasted_iota(jnp.int32, (WINDOW, 2 * WINDOW), 0)
        place_k = lax.broadcasted_iota(jnp.int32, (WINDOW, 2 * WINDOW), 1)
        banded = (place_k > place_q) & (place_k <= place_q + WINDOW)
        for i in range(m):

            def body(b):
                row = pl.multiple_of(b * WINDOW, WINDOW)
                band = keys[i, pl.ds(row, 2 * WINDOW), :]
                key, value = band[:, :HEAD], band[:, HEAD:]
                least = jnp.where((sp == 0) & (b == 0), WINDOW, 0)
                allowed = banded & (place_k >= least)
                for p in range(count):
                    at = p * pairs
                    both = query[i, pl.ds(row + WINDOW, WINDOW), pl.ds(at, pairs)]
                    results = []
                    for half in range(2):
                        one = both[:, half * HEAD : (half + 1) * HEAD]
                        scores = lax.dot_general(
                            one, key, (((1,), (1,)), ((), ())), preferred_element_type=jnp.float32
                        ) * (1.0 / HEAD**0.5)
                        scores = jnp.where(allowed, scores, -jnp.inf)
                        logit = sink[fs * heads + 2 * p + half]
                        peak = jnp.maximum(jnp.max(scores, axis=-1, keepdims=True), logit)
                        powers = jnp.exp(scores - peak)
                        norm = jnp.sum(powers, axis=-1, keepdims=True) + jnp.exp(logit - peak)
                        probs = (powers / norm).astype(jnp.bfloat16)
                        results.append(jnp.dot(probs, value, preferred_element_type=jnp.float32))
                    query[i, pl.ds(row + WINDOW, WINDOW), pl.ds(at, pairs)] = jnp.concatenate(
                        results, axis=1
                    ).astype(jnp.bfloat16)

            loop(0, blocks, body)

    def do_gate():
        def body(i, at, step):
            gate[i, :, pl.ds(at, step)] = project(i, firsts[3] + at, step)

        tiles(body)

    def do_gated():
        def body(i, at, step):
            values = project(i, firsts[4] + at, step)
            product = gate[i, :, pl.ds(at, step)].astype(jnp.float32) * values.astype(jnp.float32)
            gate[i, :, pl.ds(at, step)] = product.astype(jnp.bfloat16)

        tiles(body)

    def do_conv():
        def body(i, at, step):
            outer = project(i, firsts[5] + at, step)[WINDOW:].astype(jnp.float32)
            mixed = None
            gated = gate[i, pl.ds(WINDOW - HALO, HALO + length), pl.ds(at, step)].astype(jnp.float32)
            for which in range(TAPS):
                there = pl.multiple_of(fs * slim + at, LANES)
                tap = taps[pl.ds(which, 1), pl.ds(there, step)].astype(jnp.float32)
                low = HALO - TAPS + 1 + which
                term = tap * gated[low : low + length]
                mixed = term if mixed is None else mixed + term
            mine_conv[i, :, pl.ds(at, step)] = (outer * mixed).astype(jnp.bfloat16)

        tiles(body)

    per = max(1, LANES // across_out)
    step_out = per * across_out
    turns = chunks // per

    def term(which, left, low, count, t):
        block = jnp.concatenate([w_out[which, t * per + i] for i in range(per)], axis=1)
        return jnp.dot(left[pl.ds(low, count), :], block, preferred_element_type=jnp.float32)

    def piece_of(t):
        return pl.ds(pl.multiple_of(t * step_out, LANES), step_out)

    def do_first():
        def body(t):
            total[:, piece_of(t)] = term(0, conv, 0, length, t)

        loop(0, turns, body)

    def swap(t):
        return remote(
            partial.at[:, piece_of(t)],
            theirs.at[:, piece_of(t)],
            swap_send.at[t],
            swap_recv.at[t],
            other_core,
        )

    def work(j):
        if j == 1:
            do_keys()
        if j == 2:
            do_query()
            do_attention()
        if j == 3:
            loop(1, m, lambda e: give(1, e).start())
            keep(1)
            do_gate()
        if j == 4:
            do_gated()
        if j == 5:
            do_conv()

    for step in range(10):
        if step < 6:
            in_from_z(step)
        elif step < 8:
            from_z(step - 6)
        if 7 <= step < 9:
            from_x(step - 7)
        if 2 <= step < 8:
            in_from_y(step - 2)
            work(step - 2)
        if step == 8:
            loop(1, m, lambda e: give(0, e).start())
            keep(0)
            from_y(0)
            loop(1, m, lambda e: given(0, e).wait_recv())
            do_first()
            loop(1, m, lambda e: given(1, e).wait_recv())
        if step == 9:
            from_y(1)

    low_mine = pl.multiple_of(tp * own, LANES)
    low_other = pl.multiple_of((1 - tp) * own, LANES)

    def final(t):
        partial[:, piece_of(t)] = (
            total[pl.ds(low_other, own), piece_of(t)] + term(1, attended, low_other, own, t)
        ).astype(jnp.bfloat16)
        total[pl.ds(low_mine, own), piece_of(t)] = (
            (total[pl.ds(low_mine, own), piece_of(t)] + term(1, attended, low_mine, own, t))
            .astype(jnp.bfloat16)
            .astype(jnp.float32)
        )
        swap(t).start()

    loop(0, turns, final)

    def add(t):
        swap(t).wait()
        out[:, piece_of(t)] = (
            total[pl.ds(low_mine, own), piece_of(t)] + theirs[:, piece_of(t)].astype(jnp.float32)
        ).astype(jnp.bfloat16)

    loop(0, turns, add)

    for j in range(6):
        loop(1, m, lambda e: trade(j, e).wait_send())
        for f in range(m):
            loop(1, n, lambda d: in_z(j, d, sp * m + f, f).wait_send())

        def in_y_done(i):
            s = lax.rem(sp + 1 + i // m, n)
            in_y(j, s * m + lax.rem(fs + i, m), grp).wait_send()

        loop(0, (n - 1) * m, in_y_done)
    for j in range(2):
        loop(1, n, lambda d: along_z(j, d).wait_send())

        def x_done(d):
            s = lax.rem(sp + d, n)
            loop(1, m, lambda e: along_x(j, s, e, s * m + fs).wait_send())

        loop(0, n, x_done)
        loop(1, chunks, lambda d: along_y(j, lax.rem(mine + d, chunks), grp).wait_send())
        loop(1, m, lambda e: give(j, e).wait_send())
    loop(1, m, lambda e: rows_x(e).wait_send())
    loop(0, m, lambda f: rows_core(f).wait_send())

    @pl.when((tp == 1) & (sp < n - 1))
    def _():
        onward.wait_send()

    @pl.when((tp == 1) & (sp > 0))
    def _():
        loop(1, m, lambda e: halo_copy(halo_here(fs), fs, m + e, to_fs(e)).wait_send())
        loop(0, m, lambda f: halo_copy(halo_here(f), f, 1 + f, other_core).wait_send())


def local(
    n,
    m,
    tokens,
    norm_gain,
    w_bgate,
    w_cgate,
    w_conv_in,
    conv_taps,
    w_query,
    w_key,
    w_value,
    sink_logits,
    conv_out_weight,
    attn_out_weight,
):
    widened = tokens[0].astype(jnp.float32)
    normed = (
        widened
        * lax.rsqrt(jnp.mean(widened * widened, axis=-1, keepdims=True) + epsilon)
        * norm_gain
    ).astype(jnp.bfloat16)
    own, features = normed.shape
    span = WINDOW + 2 * own
    depth, kv = w_key.shape
    width = w_query.shape[1]
    slim = width // m
    chunks = n * m
    bf16 = jnp.bfloat16
    vmem = pl.BlockSpec(memory_space=pltpu.VMEM)
    dma = pltpu.SemaphoreType.DMA
    mixed = pl.pallas_call(
        functools.partial(kernel, n, m),
        out_shape=jax.ShapeDtypeStruct((own, features), bf16),
        in_specs=[vmem] * 10 + [pl.BlockSpec(memory_space=pltpu.SMEM)],
        out_specs=vmem,
        scratch_shapes=[
            pltpu.VMEM((chunks, depth, 2 * kv + 4 * slim), bf16),
            pltpu.VMEM((2, chunks) + conv_out_weight.shape, bf16),
            pltpu.VMEM((m, span, features), bf16),
            pltpu.VMEM((m, span, slim), bf16),
            pltpu.VMEM((m, span, 2 * HEAD), bf16),
            pltpu.VMEM((m, span, slim), bf16),
            pltpu.VMEM((m, 2 * own, slim), bf16),
            pltpu.VMEM((2 * own, width), bf16),
            pltpu.VMEM((2 * own, width), bf16),
            pltpu.VMEM((2 * own, features), jnp.float32),
            pltpu.VMEM((own, features), bf16),
            pltpu.VMEM((own, features), bf16),
            dma((9,)),
            dma((2 * m,)),
            dma((m, 2)),
            dma((2 * m,)),
            dma((m,)),
            dma((6, m)),
            dma((6, m)),
            dma((6, n, m)),
            dma((6, chunks)),
            dma((6, chunks)),
            dma((6, chunks)),
            dma((2, n)),
            dma((2, n, m)),
            dma((2, chunks)),
            dma((2, chunks)),
            dma((2, chunks)),
            dma((2, m)),
            dma((2, m)),
            dma((chunks,)),
            dma((chunks,)),
        ],
        compiler_params=pltpu.CompilerParams(
            collective_id=0, has_side_effects=True, vmem_limit_bytes=67_000_000
        ),
    )(
        normed,
        w_key,
        w_value,
        w_query,
        w_cgate,
        w_conv_in,
        w_bgate,
        conv_out_weight,
        attn_out_weight,
        conv_taps,
        sink_logits,
    )
    return mixed[None]


def solution(mesh):
    placed = (
        P(("grp", "fs"), ("sp", "tp"), None),
        P(),
        P(("sp", "fs"), "tp"),
        P(("sp", "fs"), "tp"),
        P(("sp", "fs"), "tp"),
        P(None, "tp"),
        P(("sp", "fs"), "tp"),
        P(("sp", "fs"), "tp"),
        P(("sp", "fs"), "tp"),
        P("tp"),
        P("tp", ("sp", "fs")),
        P("tp", ("sp", "fs")),
    )
    return jax.shard_map(
        functools.partial(local, mesh.shape["sp"], mesh.shape["fs"]),
        mesh=mesh,
        in_specs=placed,
        out_specs=P(("grp", "fs"), ("sp", "tp"), None),
        check_vma=False,
    )
```

```python
import functools

import jax
import jax.numpy as jnp
from jax import lax
from jax.experimental import pallas as pl
from jax.experimental.pallas import tpu as pltpu
from jax.sharding import PartitionSpec as P

HEAD = 64
WINDOW = 128
TAPS = 3
LANES = 128
HALO = 16
TILE = 256
UNIT = 16
MESH = pl.DeviceIdType.MESH

epsilon = 1e-06


def part(count, sixteenths):
    return max(UNIT, count * sixteenths // 16 // UNIT * UNIT)


def kernel(
    n,
    m,
    normed,
    w_key,
    w_value,
    w_query,
    w_cgate,
    w_conv_in,
    w_bgate,
    conv_weight,
    attn_weight,
    taps,
    sink,
    out,
    w_in,
    w_out,
    rows,
    query,
    keys,
    gate,
    mine_conv,
    conv,
    attended,
    total,
    partial,
    theirs,
    local_sem,
    rows_send,
    rows_recv,
    halo_send,
    halo_recv,
    trade_send,
    trade_recv,
    in_send,
    in_recv,
    in_on,
    in_y_send,
    in_y_recv,
    z_send,
    z_on,
    x_send,
    out_recv,
    y_send,
    y_recv,
    give_send,
    give_recv,
    swap_send,
    swap_recv,
):
    inputs = (w_key, w_value, w_query, w_cgate, w_conv_in, w_bgate)
    outputs = (conv_weight, attn_weight)
    own, features = normed.shape
    length = 2 * own
    span = WINDOW + length
    depth, kv = w_key.shape
    width = w_query.shape[1]
    slim = width // m
    across_out = conv_weight.shape[1]
    heads = slim // HEAD
    per_kv = width // kv
    chunks = n * m
    firsts = [0, kv] + [2 * kv + i * slim for i in range(4)]
    sizes = [kv, kv] + [slim] * 4
    in_alone = [part(depth, 7)] * 6
    out_alone = [part(width, 7), part(width, 5)]

    grp, sp = lax.axis_index("grp"), lax.axis_index("sp")
    fs, tp = lax.axis_index("fs"), lax.axis_index("tp")
    mine = sp * m + fs

    def loop(low, high, body):
        def step(i, carry):
            body(i)
            return carry

        lax.fori_loop(low, high, step, 0)

    def remote(source, target, send, recv, where):
        return pltpu.make_async_remote_copy(
            source, target, send, recv, device_id=where, device_id_type=MESH
        )

    def to_sp(d):
        return {"sp": lax.rem(sp + d, n)}

    def to_fs(e):
        return {"fs": lax.rem(fs + e, m)}

    other_core = {"tp": 1 - tp}
    other_grp = {"grp": 1 - grp}

    def columns(j, f):
        if j < 2:
            return pl.ds(0, kv)
        return pl.ds(pl.multiple_of(f * slim, LANES), slim)

    def kept(j):
        return pl.ds(firsts[j], sizes[j])

    fills = [
        pltpu.make_async_copy(
            inputs[j].at[:, columns(j, fs)], w_in.at[mine, :, kept(j)], local_sem.at[j]
        )
        for j in range(6)
    ] + [
        pltpu.make_async_copy(outputs[j], w_out.at[j, mine], local_sem.at[6 + j]) for j in range(2)
    ]
    at_own = pl.multiple_of(WINDOW + tp * own, LANES)
    at_other = pl.multiple_of(WINDOW + (1 - tp) * own, LANES)
    fills.append(
        pltpu.make_async_copy(normed, rows.at[fs, pl.ds(at_own, own)], local_sem.at[8])
    )
    for fill in fills:
        fill.start()

    @pl.when(sp == 0)
    def _():
        for i in range(m):
            rows[i, pl.ds(0, WINDOW), :] = jnp.zeros((WINDOW, features), jnp.bfloat16)

    barrier = pltpu.get_barrier_semaphore()

    def greet(where):
        pl.semaphore_signal(barrier, inc=1, device_id=where, device_id_type=MESH)

    loop(1, n, lambda d: greet(to_sp(d)))
    loop(1, m, lambda e: greet(to_fs(e)))
    greet(other_grp)
    greet(other_core)
    pl.semaphore_wait(barrier, n + m)

    def trade(j, e):
        f = lax.rem(fs + e, m)
        return remote(
            inputs[j].at[:, columns(j, f)],
            w_in.at[mine, :, kept(j)],
            trade_send.at[j, e],
            trade_recv.at[j, fs],
            {"fs": f},
        )

    def trade_arrival(j, f):
        piece = w_in.at[sp * m + f, :, kept(j)]
        return remote(piece, piece, trade_send.at[j, 0], trade_recv.at[j, f], to_fs(1))

    def in_rows(j):
        return pl.ds(pl.multiple_of(grp * in_alone[j], UNIT), depth - in_alone[j])

    def in_lone(j, group):
        return pl.ds(
            pl.multiple_of(group * (depth - in_alone[j]), UNIT), in_alone[j]
        )

    steps = (1, -1, 2, -2)

    def near(body):
        for slot, by in enumerate(steps):
            there = sp + by

            @pl.when((there >= 0) & (there < n))
            def _():
                body(slot, jnp.clip(there, 0, n - 1))

    def hand_on(s, body):
        @pl.when((sp - s >= 2) & (sp < n - 1))
        def _():
            body(jnp.minimum(sp + 1, n - 1))

        @pl.when((s - sp >= 2) & (sp > 0))
        def _():
            body(jnp.maximum(sp - 1, 0))

    def other_sp(d):
        return lax.rem(jnp.where(2 * sp >= n, sp - d + n, sp + d), n)

    def in_z(j, slot, chunk, f, there):
        piece = w_in.at[chunk, in_rows(j), kept(j)]
        return remote(
            piece, piece, in_send.at[j, slot, f], in_recv.at[j, chunk], {"sp": there}
        )

    def in_hand(j, chunk, there):
        piece = w_in.at[chunk, in_rows(j), kept(j)]
        return remote(piece, piece, in_on.at[j, chunk], in_recv.at[j, chunk], {"sp": there})

    def in_y(j, chunk, group):
        piece = w_in.at[chunk, in_lone(j, group), kept(j)]
        return remote(piece, piece, in_y_send.at[j, chunk], in_y_recv.at[j, chunk], other_grp)

    def rows_copy(source, f, core, send, where):
        at = pl.multiple_of(WINDOW + core * own, LANES)
        return remote(
            source, rows.at[f, pl.ds(at, own)], rows_send.at[send], rows_recv.at[f, core], where
        )

    def rows_x(e):
        return rows_copy(normed, fs, tp, e, to_fs(e))

    def rows_core(f):
        return rows_copy(rows.at[f, pl.ds(at_own, own)], f, tp, m + f, other_core)

    def halo_copy(source, f, send, where):
        return remote(
            source, rows.at[f, pl.ds(0, WINDOW)], halo_send.at[send], halo_recv.at[f], where
        )

    def halo_here(f):
        return rows.at[f, pl.ds(0, WINDOW)]

    onward = halo_copy(normed.at[pl.ds(own - WINDOW, WINDOW)], fs, 0, to_sp(1))

    def out_rows(j):
        return pl.ds(pl.multiple_of(grp * out_alone[j], UNIT), width - out_alone[j])

    def out_lone(j, group):
        return pl.ds(pl.multiple_of(group * (width - out_alone[j]), UNIT), out_alone[j])

    def along_z(j, slot, there):
        piece = w_out.at[j, mine, out_rows(j)]
        return remote(piece, piece, z_send.at[j, slot], out_recv.at[j, mine], {"sp": there})

    def out_hand(j, chunk, there):
        piece = w_out.at[j, chunk, out_rows(j)]
        return remote(piece, piece, z_on.at[j, chunk], out_recv.at[j, chunk], {"sp": there})

    def along_x(j, s, e, chunk):
        piece = w_out.at[j, chunk, out_rows(j)]
        return remote(piece, piece, x_send.at[j, s, e], out_recv.at[j, chunk], to_fs(e))

    def arrival(j, chunk):
        piece = w_out.at[j, chunk, out_rows(j)]
        return remote(piece, piece, z_send.at[j, 0], out_recv.at[j, chunk], to_sp(1))

    def along_y(j, chunk, group):
        piece = w_out.at[j, chunk, out_lone(j, group)]
        return remote(piece, piece, y_send.at[j, chunk], y_recv.at[j, chunk], other_grp)

    def own_in(j):
        fills[j].wait()
        near(lambda slot, there: in_z(j, slot, mine, fs, there).start())

    def traded_in(j):
        def traded(e):
            f = lax.rem(fs + e, m)
            trade_arrival(j, f).wait_recv()
            near(lambda slot, there: in_z(j, slot, sp * m + f, f, there).start())

        loop(1, m, traded)

    def own_out(j):
        fills[6 + j].wait()
        near(lambda slot, there: along_z(j, slot, there).start())
        loop(1, m, lambda e: along_x(j, sp, e, mine).start())

    for j in range(3):
        loop(1, m, lambda e: trade(j, e).start())
        own_in(j)

    @pl.when((tp == 1) & (sp < n - 1))
    def _():
        onward.start()

    loop(1, m, lambda e: rows_x(e).start())
    for j in range(3, 6):
        loop(1, m, lambda e: trade(j, e).start())
    fills[8].wait()
    rows_core(fs).start()
    for j in range(3):
        traded_in(j)
    own_in(3)
    own_out(0)
    own_in(4)
    traded_in(3)
    own_in(5)
    traded_in(4)
    traded_in(5)
    own_out(1)

    def rows_on(e):
        f = lax.rem(fs + e, m)
        rows_copy(rows.at[f, pl.ds(at_own, own)], f, tp, 0, to_fs(e)).wait_recv()
        rows_core(f).start()

    loop(1, m, rows_on)

    @pl.when((tp == 1) & (sp > 0))
    def _():
        halo_copy(halo_here(fs), fs, 0, other_core).wait_recv()
        halo_copy(halo_here(fs), fs, 1 + fs, other_core).start()
        loop(1, m, lambda e: halo_copy(halo_here(fs), fs, m + e, to_fs(e)).start())

        def pass_on(e):
            f = lax.rem(fs + e, m)
            halo_copy(halo_here(f), f, 0, other_core).wait_recv()
            halo_copy(halo_here(f), f, 1 + f, other_core).start()

        loop(1, m, pass_on)

    def rows_in(f):
        piece = rows.at[f, pl.ds(at_other, own)]
        remote(piece, piece, rows_send.at[0], rows_recv.at[f, 1 - tp], other_core).wait_recv()

    loop(0, m, rows_in)

    @pl.when((tp == 0) & (sp > 0))
    def _():
        loop(0, m, lambda f: halo_copy(halo_here(f), f, 0, other_core).wait_recv())

    def in_from_z(j):
        def body(i):
            s = other_sp(1 + i // m)
            chunk = s * m + lax.rem(fs + i, m)
            in_hand(j, chunk, sp).wait_recv()
            hand_on(s, lambda there: in_hand(j, chunk, there).start())
            in_y(j, chunk, grp).start()

        loop(0, (n - 1) * m, body)

    def in_from_y(j):
        def body(i):
            s = other_sp(1 + i // m)
            in_y(j, s * m + lax.rem(fs + i, m), 1 - grp).wait_recv()

        loop(0, (n - 1) * m, body)

    def from_z(j):
        def body(d):
            s = other_sp(d)
            chunk = s * m + fs
            arrival(j, chunk).wait_recv()
            hand_on(s, lambda there: out_hand(j, chunk, there).start())
            loop(1, m, lambda e: along_x(j, s, e, chunk).start())
            along_y(j, chunk, grp).start()

        loop(1, n, body)

    def from_x(j):
        def body(d):
            s = lax.rem(sp + d, n)

            def inner(e):
                chunk = s * m + lax.rem(fs + e, m)
                arrival(j, chunk).wait_recv()
                along_y(j, chunk, grp).start()

            loop(1, m, inner)

        loop(0, n, body)

    def from_y(j):
        loop(
            1,
            chunks,
            lambda d: along_y(j, lax.rem(mine + d, chunks), 1 - grp).wait_recv(),
        )

    def project(i, first, count):
        block = w_in[:, :, pl.ds(first, count)].reshape(chunks * depth, count)
        return jnp.dot(rows[i], block, preferred_element_type=jnp.float32).astype(jnp.bfloat16)

    def tiles(body):
        step = min(TILE, slim)
        for i in range(m):
            loop(0, slim // step, lambda t: body(i, pl.multiple_of(t * step, LANES), step))

    kv_head = fs * heads // per_kv

    def do_keys():
        for i in range(m):
            both = project(i, 0, 2 * kv).astype(jnp.float32)
            picked = []
            for base in (0, kv):
                one = both[:, base : base + HEAD]
                for h in range(1, kv // HEAD):
                    at = base + h * HEAD
                    one = jnp.where(kv_head == h, both[:, at : at + HEAD], one)
                picked.append(one)
            keys[i] = jnp.concatenate(picked, axis=1).astype(jnp.bfloat16)

    def do_query():
        def body(i, at, step):
            query[i, :, pl.ds(at, step)] = project(i, firsts[2] + at, step)

        tiles(body)

    def result(which, f):
        return mine_conv.at[f] if which == 0 else query.at[f, pl.ds(WINDOW, length)]

    def give(which, e):
        full = (conv, attended)[which]
        f = lax.rem(fs + e, m)
        here = pl.ds(pl.multiple_of(fs * slim, LANES), slim)
        return remote(
            result(which, f), full.at[:, here], give_send.at[which, e], give_recv.at[which, fs], {"fs": f}
        )

    def given(which, e):
        full = (conv, attended)[which]
        f = lax.rem(fs + e, m)
        piece = full.at[:, pl.ds(pl.multiple_of(f * slim, LANES), slim)]
        return remote(piece, piece, give_send.at[which, 0], give_recv.at[which, f], to_fs(e))

    def keep(which):
        full = (conv, attended)[which]
        full[:, pl.ds(pl.multiple_of(fs * slim, LANES), slim)] = result(which, fs)[...]

    def do_attention():
        pairs = 2 * HEAD
        blocks = length // WINDOW
        count = heads // 2
        place_q = lax.broadcasted_iota(jnp.int32, (WINDOW, 2 * WINDOW), 0)
        place_k = lax.broadcasted_iota(jnp.int32, (WINDOW, 2 * WINDOW), 1)
        banded = (place_k > place_q) & (place_k <= place_q + WINDOW)
        for i in range(m):

            def body(b):
                row = pl.multiple_of(b * WINDOW, WINDOW)
                band = keys[i, pl.ds(row, 2 * WINDOW), :]
                key, value = band[:, :HEAD], band[:, HEAD:]
                least = jnp.where((sp == 0) & (b == 0), WINDOW, 0)
                allowed = banded & (place_k >= least)
                for p in range(count):
                    at = p * pairs
                    both = query[i, pl.ds(row + WINDOW, WINDOW), pl.ds(at, pairs)]
                    results = []
                    for half in range(2):
                        one = both[:, half * HEAD : (half + 1) * HEAD]
                        scores = lax.dot_general(
                            one, key, (((1,), (1,)), ((), ())), preferred_element_type=jnp.float32
                        ) * (1.0 / HEAD**0.5)
                        scores = jnp.where(allowed, scores, -jnp.inf)
                        logit = sink[fs * heads + 2 * p + half]
                        peak = jnp.maximum(jnp.max(scores, axis=-1, keepdims=True), logit)
                        powers = jnp.exp(scores - peak)
                        norm = jnp.sum(powers, axis=-1, keepdims=True) + jnp.exp(logit - peak)
                        probs = (powers / norm).astype(jnp.bfloat16)
                        results.append(jnp.dot(probs, value, preferred_element_type=jnp.float32))
                    query[i, pl.ds(row + WINDOW, WINDOW), pl.ds(at, pairs)] = jnp.concatenate(
                        results, axis=1
                    ).astype(jnp.bfloat16)

            loop(0, blocks, body)

    def do_gate():
        def body(i, at, step):
            gate[i, :, pl.ds(at, step)] = project(i, firsts[3] + at, step)

        tiles(body)

    def do_gated():
        def body(i, at, step):
            values = project(i, firsts[4] + at, step)
            product = gate[i, :, pl.ds(at, step)].astype(jnp.float32) * values.astype(jnp.float32)
            gate[i, :, pl.ds(at, step)] = product.astype(jnp.bfloat16)

        tiles(body)

    def do_conv():
        def body(i, at, step):
            outer = project(i, firsts[5] + at, step)[WINDOW:].astype(jnp.float32)
            mixed = None
            gated = gate[i, pl.ds(WINDOW - HALO, HALO + length), pl.ds(at, step)].astype(jnp.float32)
            for which in range(TAPS):
                there = pl.multiple_of(fs * slim + at, LANES)
                tap = taps[pl.ds(which, 1), pl.ds(there, step)].astype(jnp.float32)
                low = HALO - TAPS + 1 + which
                term = tap * gated[low : low + length]
                mixed = term if mixed is None else mixed + term
            mine_conv[i, :, pl.ds(at, step)] = (outer * mixed).astype(jnp.bfloat16)

        tiles(body)

    per = max(1, LANES // across_out)
    step_out = per * across_out
    turns = chunks // per

    def term(which, left, low, count, t):
        block = jnp.concatenate([w_out[which, t * per + i] for i in range(per)], axis=1)
        return jnp.dot(left[pl.ds(low, count), :], block, preferred_element_type=jnp.float32)

    def piece_of(t):
        return pl.ds(pl.multiple_of(t * step_out, LANES), step_out)

    def do_first():
        def body(t):
            total[:, piece_of(t)] = term(0, conv, 0, length, t)

        loop(0, turns, body)

    def swap(t):
        return remote(
            partial.at[:, piece_of(t)],
            theirs.at[:, piece_of(t)],
            swap_send.at[t],
            swap_recv.at[t],
            other_core,
        )

    def work(j):
        if j == 1:
            do_keys()
        if j == 2:
            do_query()
            do_attention()
        if j == 3:
            loop(1, m, lambda e: give(1, e).start())
            keep(1)
            do_gate()
        if j == 4:
            do_gated()
        if j == 5:
            do_conv()

    order = (0, 1, 2, 3, 6, 4, 5, 7)
    for step in range(10):
        if step < 8:
            item = order[step]
            in_from_z(item) if item < 6 else from_z(item - 6)
        if 1 <= step < 9 and order[step - 1] >= 6:
            from_x(order[step - 1] - 6)
        if step >= 2:
            item = order[step - 2]
            if item < 6:
                in_from_y(item)
                work(item)
            elif item == 6:
                from_y(0)
            else:
                loop(1, m, lambda e: given(0, e).wait_recv())
                do_first()
                loop(1, m, lambda e: given(1, e).wait_recv())
                from_y(1)
        if step == 8:
            loop(1, m, lambda e: give(0, e).start())
            keep(0)

    low_mine = pl.multiple_of(tp * own, LANES)
    low_other = pl.multiple_of((1 - tp) * own, LANES)

    def final(t):
        partial[:, piece_of(t)] = (
            total[pl.ds(low_other, own), piece_of(t)] + term(1, attended, low_other, own, t)
        ).astype(jnp.bfloat16)
        total[pl.ds(low_mine, own), piece_of(t)] = (
            (total[pl.ds(low_mine, own), piece_of(t)] + term(1, attended, low_mine, own, t))
            .astype(jnp.bfloat16)
            .astype(jnp.float32)
        )
        swap(t).start()

    loop(0, turns, final)

    def add(t):
        swap(t).wait()
        out[:, piece_of(t)] = (
            total[pl.ds(low_mine, own), piece_of(t)] + theirs[:, piece_of(t)].astype(jnp.float32)
        ).astype(jnp.bfloat16)

    loop(0, turns, add)

    for j in range(6):
        loop(1, m, lambda e: trade(j, e).wait_send())
        for f in range(m):
            near(lambda slot, there: in_z(j, slot, sp * m + f, f, there).wait_send())

        def in_y_done(i):
            s = other_sp(1 + i // m)
            chunk = s * m + lax.rem(fs + i, m)
            in_y(j, chunk, grp).wait_send()
            hand_on(s, lambda there: in_hand(j, chunk, there).wait_send())

        loop(0, (n - 1) * m, in_y_done)
    for j in range(2):
        near(lambda slot, there: along_z(j, slot, there).wait_send())

        def x_done(d):
            s = lax.rem(sp + d, n)
            hand_on(s, lambda there: out_hand(j, s * m + fs, there).wait_send())
            loop(1, m, lambda e: along_x(j, s, e, s * m + fs).wait_send())

        loop(0, n, x_done)
        loop(1, chunks, lambda d: along_y(j, lax.rem(mine + d, chunks), grp).wait_send())
        loop(1, m, lambda e: give(j, e).wait_send())
    loop(1, m, lambda e: rows_x(e).wait_send())
    loop(0, m, lambda f: rows_core(f).wait_send())

    @pl.when((tp == 1) & (sp < n - 1))
    def _():
        onward.wait_send()

    @pl.when((tp == 1) & (sp > 0))
    def _():
        loop(1, m, lambda e: halo_copy(halo_here(fs), fs, m + e, to_fs(e)).wait_send())
        loop(0, m, lambda f: halo_copy(halo_here(f), f, 1 + f, other_core).wait_send())


def local(
    n,
    m,
    tokens,
    norm_gain,
    w_bgate,
    w_cgate,
    w_conv_in,
    conv_taps,
    w_query,
    w_key,
    w_value,
    sink_logits,
    conv_out_weight,
    attn_out_weight,
):
    widened = tokens[0].astype(jnp.float32)
    normed = (
        widened
        * lax.rsqrt(jnp.mean(widened * widened, axis=-1, keepdims=True) + epsilon)
        * norm_gain
    ).astype(jnp.bfloat16)
    own, features = normed.shape
    span = WINDOW + 2 * own
    depth, kv = w_key.shape
    width = w_query.shape[1]
    slim = width // m
    chunks = n * m
    bf16 = jnp.bfloat16
    vmem = pl.BlockSpec(memory_space=pltpu.VMEM)
    dma = pltpu.SemaphoreType.DMA
    mixed = pl.pallas_call(
        functools.partial(kernel, n, m),
        out_shape=jax.ShapeDtypeStruct((own, features), bf16),
        in_specs=[vmem] * 10 + [pl.BlockSpec(memory_space=pltpu.SMEM)],
        out_specs=vmem,
        scratch_shapes=[
            pltpu.VMEM((chunks, depth, 2 * kv + 4 * slim), bf16),
            pltpu.VMEM((2, chunks) + conv_out_weight.shape, bf16),
            pltpu.VMEM((m, span, features), bf16),
            pltpu.VMEM((m, span, slim), bf16),
            pltpu.VMEM((m, span, 2 * HEAD), bf16),
            pltpu.VMEM((m, span, slim), bf16),
            pltpu.VMEM((m, 2 * own, slim), bf16),
            pltpu.VMEM((2 * own, width), bf16),
            pltpu.VMEM((2 * own, width), bf16),
            pltpu.VMEM((2 * own, features), jnp.float32),
            pltpu.VMEM((own, features), bf16),
            pltpu.VMEM((own, features), bf16),
            dma((9,)),
            dma((2 * m,)),
            dma((m, 2)),
            dma((2 * m,)),
            dma((m,)),
            dma((6, m)),
            dma((6, m)),
            dma((6, 4, m)),
            dma((6, chunks)),
            dma((6, chunks)),
            dma((6, chunks)),
            dma((6, chunks)),
            dma((2, 4)),
            dma((2, chunks)),
            dma((2, n, m)),
            dma((2, chunks)),
            dma((2, chunks)),
            dma((2, chunks)),
            dma((2, m)),
            dma((2, m)),
            dma((chunks,)),
            dma((chunks,)),
        ],
        compiler_params=pltpu.CompilerParams(
            collective_id=0, has_side_effects=True, vmem_limit_bytes=67_000_000
        ),
    )(
        normed,
        w_key,
        w_value,
        w_query,
        w_cgate,
        w_conv_in,
        w_bgate,
        conv_out_weight,
        attn_out_weight,
        conv_taps,
        sink_logits,
    )
    return mixed[None]


def solution(mesh):
    placed = (
        P(("grp", "fs"), ("sp", "tp"), None),
        P(),
        P(("sp", "fs"), "tp"),
        P(("sp", "fs"), "tp"),
        P(("sp", "fs"), "tp"),
        P(None, "tp"),
        P(("sp", "fs"), "tp"),
        P(("sp", "fs"), "tp"),
        P(("sp", "fs"), "tp"),
        P("tp"),
        P("tp", ("sp", "fs")),
        P("tp", ("sp", "fs")),
    )
    return jax.shard_map(
        functools.partial(local, mesh.shape["sp"], mesh.shape["fs"]),
        mesh=mesh,
        in_specs=placed,
        out_specs=P(("grp", "fs"), ("sp", "tp"), None),
        check_vma=False,
    )
```
